32 devices in a mesh: kv: 8 (over z, x), tp: 4 (over y, core).
Axes of the slice: x: 2, y: 2, z: 4, core: 2. Of those that a mesh axis runs over, the one named last changes fastest.
Arguments:
- inputs: bfloat16 [4, 2048, 2048], P(None, 'kv'), may hold values from -40 to 40
- query_weight: bfloat16 [2048, 2048], P(None, 'tp'), may hold values from -0.125 to 0.125
- key_weight: bfloat16 [2048, 1024], P(None, 'tp'), may hold values from -0.125 to 0.125
- value_weight: bfloat16 [2048, 1024], P(None, 'tp'), may hold values from -0.125 to 0.125
- out_weight: bfloat16 [2048, 2048], P('tp'), may hold values from -1 to 1
- chosen: int32 [4, 32, 32], P(None, 'kv'), may hold values from 0 to 31, as said below
- lengths: int32 [4], replicated, may hold values from 1 to 2048, 3072 in all
Outputs:
- mixed: bfloat16 [4, 2048, 2048], P(None, 'kv', 'tp')
The draws below stay inside these ranges and needn't reach their ends.
Inputs may be any that keep to these rules, and one draw needn't show every extreme that they name: chosen[b, q, 0] = q; every entry names a block of the same sequence at or before q; entries may repeat. Over the query blocks of positions k * 256 to (k+1) * 256 - 1 of all sequences, the named blocks that lie in another span of 256 positions number at most 3 distinct blocks for each other span, and 3 is reached.
All inputs are finite; a program needn't handle non-finite values.
Results may differ from the reference program's by a relative error of at most 0.014.
The reference program's roundings to bfloat16 on the way count: a program that leaves them out, or rounds other values in their place, can miss the bound.
Values may be sent and summed in bfloat16 or wider, within the bound.
A program may use at most 128 MiB of HBM per device.

```python
import math
import jax
import jax.numpy as jnp
import numpy as np
from jax import lax

D = 2048
HEADS = 16
KV_HEADS = 8
HD = 128
KB = 64
TOPK = 32
CAP = 3
BATCH = 4
SEQ_DEV = 256
SEQ = 2048
NB = 32
N_TP = 4


def draw_inputs(key, part):
    key_base = jax.random.fold_in(jax.random.fold_in(key, 3), 0)
    entries = jax.random.normal(key_base, (BATCH, SEQ, D), jnp.float32)
    return jnp.clip(entries, -40.0, 40.0).astype(jnp.bfloat16)


def draw_chosen(key, part):
    per_dev = SEQ_DEV // KB
    ndevices = NB // per_dev
    owned = BATCH * per_dev
    key_count, key_rank, key_order = jax.random.split(jax.random.fold_in(key, 7), 3)
    receiver = jnp.arange(ndevices, dtype=jnp.int32)[:, None]
    sender = jnp.arange(ndevices, dtype=jnp.int32)[None, :]
    counts = jax.random.randint(key_count, (ndevices, ndevices), 1, CAP + 1)
    counts = jnp.where(sender == receiver - 1, CAP, counts)
    counts = jnp.where(sender < receiver, counts, 0)
    local_ids = jnp.arange(owned, dtype=jnp.int32)
    noise = jax.random.randint(key_rank, (ndevices, ndevices, owned), 0, 1 << 20) * owned + local_ids
    ranks = jnp.argsort(jnp.argsort(noise, axis=-1), axis=-1)
    picked = ranks < counts[:, :, None]
    order_noise = jax.random.randint(key_order, (ndevices, ndevices), 0, 1 << 20) * ndevices + sender
    priority = jnp.argsort(jnp.argsort(order_noise, axis=-1), axis=-1) + 2
    priority = jnp.where(sender == receiver - ndevices // 2, 1, priority)
    priority = jnp.where(sender == receiver - 1, 0, priority)
    seq_of = local_ids // per_dev
    global_block = sender[:, :, None] * per_dev + (local_ids % per_dev)[None, None, :]
    big_score = (ndevices + 4) * owned
    seq_range = jnp.arange(BATCH, dtype=jnp.int32)
    in_seq = picked[:, None, :, :] & (seq_of[None, None, None, :] == seq_range[None, :, None, None])
    scored = jnp.where(in_seq, priority[:, None, :, None] * owned + local_ids[None, None, None, :], big_score)
    scored = scored.reshape(ndevices, BATCH, ndevices * owned)
    sorted_idx = jnp.argsort(scored, axis=-1)
    pool_size = jnp.sum(in_seq.reshape(ndevices, BATCH, ndevices * owned).astype(jnp.int32), axis=-1)
    pool_blocks = jnp.take_along_axis(jnp.broadcast_to(global_block.reshape(1, 1, ndevices * owned), (ndevices, BATCH, ndevices * owned)), sorted_idx, axis=-1)
    local_row = jnp.arange(per_dev, dtype=jnp.int32)[:, None]
    slot_col = jnp.arange(TOPK, dtype=jnp.int32)[None, :]
    base_count = local_row * (TOPK - 1) - local_row * (local_row - 1) // 2
    counter = base_count + slot_col - 1 - local_row
    safe_size = jnp.maximum(pool_size, 1)
    pool_pick = jnp.take_along_axis(pool_blocks, counter.reshape(1, 1, -1) % safe_size[:, :, None], axis=-1)
    pool_pick = pool_pick.reshape(ndevices, BATCH, per_dev, TOPK)
    own_block = jnp.arange(ndevices, dtype=jnp.int32)[:, None, None, None] * per_dev + local_row[None, None, :, :] + 0 * slot_col[None, None, :, :]
    earlier = own_block - local_row[None, None, :, :] + slot_col[None, None, :, :] - 1
    result = jnp.where(pool_size[:, :, None, None] > 0, pool_pick, own_block)
    result = jnp.where((slot_col >= 1) & (slot_col <= local_row), earlier, result)
    result = jnp.where(slot_col == 0, own_block, result)
    return jnp.transpose(result, (1, 0, 2, 3)).reshape(BATCH, NB, TOPK).astype(jnp.int32)


def level_of(stream_key, dims, cuts, smallest, largest):
    level = 1.0
    for dim, parts in cuts:
        steps = jax.random.uniform(jax.random.fold_in(jax.random.fold_in(stream_key, 6), dim), (parts,), jnp.float32, smallest / len(cuts), largest / len(cuts))
        level = level * jnp.repeat(jnp.exp(steps), dims[dim] // parts).reshape((-1,) + (1,) * (len(dims) - 1 - dim))
    return level


def profile(count, total, reach, lean):
    portions = [(1 << 20) // math.isqrt(grade ** lean) + 1 for grade in range(2, count + 1)]
    surplus, given = total - reach - (count - 1), [1] * (count - 1)
    while surplus > 0:
        candidates = [i for i in range(count - 1) if given[i] < reach]
        mass, budget = sum([portions[i] for i in candidates]), surplus
        for i in candidates:
            addition = min(reach - given[i], max(1, budget * portions[i] // mass), surplus)
            given[i] = given[i] + addition
            surplus = surplus - addition
    return np.array([reach] + given)


def uneven(key, amount, total, bound, slope):
    if amount == 2:
        one = jax.random.randint(key, (), max(1, total - bound), min(bound, total - 1) + 1)
        return jnp.stack([one, total - one])
    tallies = jnp.asarray(profile(amount, total, bound, slope), jnp.int32)
    pairs = (amount - 1) // 2
    source_of, taker = tallies[1:1 + 2 * pairs:2], tallies[2:2 + 2 * pairs:2]
    margin = jnp.minimum(source_of - 1, bound - taker)
    moved = jax.random.randint(jax.random.fold_in(key, 1), (pairs,), 0, 1 << 20) % (margin + 1)
    tallies = tallies.at[1:1 + 2 * pairs:2].set(source_of - moved).at[2:2 + 2 * pairs:2].set(taker + moved)
    return tallies[jax.random.permutation(jax.random.fold_in(key, 2), amount)]


def gaussian(stream_key, extent, spread, bound, pieces=(), kind=jnp.bfloat16):
    array = jax.random.normal(stream_key, extent, jnp.float32) * spread
    if len(pieces) > 0:
        array = level_of(stream_key, extent, pieces, -0.22, 0.18) * array
    return jnp.clip(array, min=-bound, max=bound).astype(kind)


def setup_inputs(seed: int = 0) -> dict:
    seeds = jax.random.split(jax.random.key(seed), 8)
    return {
        "inputs": draw_inputs(jax.random.fold_in(seeds[7], 71), 0),
        "query_weight": gaussian(seeds[1], (D, HEADS * HD), D ** -0.5, 0.125, ((1, 4),)),
        "key_weight": gaussian(seeds[2], (D, KV_HEADS * HD), D ** -0.5, 0.125, ((1, 4),)),
        "value_weight": gaussian(seeds[3], (D, KV_HEADS * HD), D ** -0.5, 0.125, ((1, 4),)),
        "out_weight": gaussian(seeds[4], (HEADS * HD, D), (HEADS * HD // 64) ** -0.5, 1.0, ((0, 4),)),
        "chosen": draw_chosen(jax.random.fold_in(seeds[7], 71), 0),
        "lengths": uneven(seeds[6], BATCH, SEQ + SEQ // 2, SEQ, 2).astype(jnp.int32),
    }


def unique_slots(chosen_rows):
    order = jnp.arange(TOPK, dtype=jnp.int32)
    repeated = jnp.any((chosen_rows[..., :, None] == chosen_rows[..., None, :]) & (order[:, None] > order[None, :]), axis=-1)
    return jnp.repeat(jnp.logical_not(repeated), KB, axis=-1)


def attend(queries, key_sets, value_sets, key_pos, unique_key, query_pos, live_length):
    scores = jnp.einsum("nqkgd,npkd->nkgqp", queries.astype(jnp.float32), key_sets.astype(jnp.float32)) * (HD ** -0.5)
    allowed = (key_pos[:, None, :] <= query_pos[:, :, None]) & (key_pos[:, None, :] < live_length) & unique_key[:, None, :]
    allowed = allowed | (key_pos[:, None, :] == query_pos[:, :, None])
    scores = jnp.where(allowed[:, None, None], scores, -jnp.inf)
    highest = jnp.max(scores, axis=-1, keepdims=True)
    raised = jnp.exp(scores - highest)
    weights = (raised / jnp.sum(raised, axis=-1, keepdims=True)).astype(jnp.bfloat16)
    combined = jnp.einsum("nkgqp,npkd->nqkgd", weights.astype(jnp.float32), value_sets.astype(jnp.float32))
    living = (query_pos < live_length)[:, :, None, None, None]
    return jnp.where(living, combined, 0.0).astype(jnp.bfloat16)


def reference(inputs, query_weight, key_weight, value_weight, out_weight, chosen, lengths):
    per_group = HEADS // KV_HEADS
    flat_rows = inputs.reshape(BATCH * SEQ, D)
    queries = jnp.dot(flat_rows, query_weight, preferred_element_type=jnp.float32).astype(jnp.bfloat16)
    queries = queries.reshape(BATCH, NB, KB, KV_HEADS, per_group, HD)
    key_rows = jnp.dot(flat_rows, key_weight, preferred_element_type=jnp.float32).astype(jnp.bfloat16)
    key_rows = key_rows.reshape(BATCH, NB, KB, KV_HEADS, HD)
    value_rows = jnp.dot(flat_rows, value_weight, preferred_element_type=jnp.float32).astype(jnp.bfloat16)
    value_rows = value_rows.reshape(BATCH, NB, KB, KV_HEADS, HD)
    offsets = jnp.arange(KB, dtype=jnp.int32)

    def one_block(block_pair):
        seq_index, block_id = block_pair
        names = chosen[seq_index, block_id]
        key_sets = key_rows[seq_index][names].reshape(1, TOPK * KB, KV_HEADS, HD)
        value_sets = value_rows[seq_index][names].reshape(1, TOPK * KB, KV_HEADS, HD)
        key_pos = (names[:, None] * KB + offsets[None, :]).reshape(1, TOPK * KB)
        query_pos = (block_id * KB + offsets)[None, :]
        unique_key = unique_slots(names)[None, :]
        result = attend(queries[seq_index, block_id][None], key_sets, value_sets, key_pos, unique_key, query_pos, lengths[seq_index])
        return result[0]

    seq_ids = jnp.repeat(jnp.arange(BATCH, dtype=jnp.int32), NB)
    block_ids = jnp.tile(jnp.arange(NB, dtype=jnp.int32), BATCH)
    attended = lax.map(one_block, (seq_ids, block_ids)).reshape(BATCH * SEQ, HEADS * HD)
    group_width = HEADS * HD // N_TP
    summed = jnp.zeros((BATCH * SEQ, D), jnp.float32)
    for group_id in range(N_TP):
        partial_value = jnp.dot(attended[:, group_id * group_width:(group_id + 1) * group_width],
                          out_weight[group_id * group_width:(group_id + 1) * group_width],
                          preferred_element_type=jnp.float32).astype(jnp.bfloat16)
        summed = summed + lax.optimization_barrier(partial_value).astype(jnp.float32)
    return summed.astype(jnp.bfloat16).reshape(BATCH, SEQ, D)
```

```python
import functools

import jax
import jax.numpy as jnp
from jax import lax
from jax.experimental import pallas as pl
from jax.experimental.pallas import tpu as pltpu
from jax.sharding import PartitionSpec as P

HD = 128
KB = 64
CAP = 3
MASKED = -1e30


def tables(chosen, devices, device):
    batch_size, per_dev, _ = chosen.shape
    blocks = jnp.arange(devices * per_dev, dtype=jnp.int32)
    named = jnp.any(chosen[..., None] == blocks, axis=2)
    named = named.reshape(batch_size, per_dev, devices, per_dev)
    own = jnp.sum(
        jnp.where(jnp.arange(devices)[None, None, :, None] == device, named, False), axis=2
    )
    needed = jnp.any(named, axis=1) & (jnp.arange(devices)[None, :, None] != device)
    needed = jnp.transpose(needed, (1, 0, 2)).reshape(devices, batch_size * per_dev)
    local = jnp.arange(batch_size * per_dev, dtype=jnp.int32)
    slots = jnp.sum(
        jnp.where(local[None, :, None] > local[None, None, :], needed[:, None, :], False),
        axis=2,
        dtype=jnp.int32,
    )
    matches = needed[:, :, None] & (slots[:, :, None] == jnp.arange(CAP, dtype=jnp.int32))
    requests = jnp.sum(jnp.where(matches, local[None, :, None], 0), axis=1)
    matches = matches.reshape(devices, batch_size, per_dev, CAP)
    matches = jnp.transpose(matches, (1, 0, 2, 3))
    remote = jnp.any(named[..., None] & matches[:, None], axis=3)
    own_bias = jnp.where(own > 0, 0.0, MASKED).astype(jnp.float32)
    own_bias = jnp.repeat(own_bias, KB, axis=-1)
    home = device * per_dev + jnp.arange(per_dev, dtype=jnp.int32)
    copies = jnp.sum(chosen == home[None, :, None], axis=-1, dtype=jnp.int32)
    same = jnp.log(jnp.maximum(copies, 1).astype(jnp.float32))
    same = jnp.broadcast_to(same[..., None], own_bias.shape)
    rem_bias = jnp.where(remote, 0.0, MASKED).astype(jnp.float32)
    rem_bias = rem_bias.reshape(batch_size, per_dev, devices // 2, 2 * CAP)
    rem_bias = jnp.repeat(jnp.transpose(rem_bias, (2, 0, 1, 3)), KB, axis=-1)
    return requests, jnp.stack([own_bias, same]), rem_bias


def attend_kernel(
    positions, kv_local, per_group, length_ref, q_ref, k_ref, v_ref, rk_ref, rv_ref,
    own_bias_ref, rem_bias_ref, out_ref, scores_ref
):
    device = lax.axis_index("kv")
    batch_size = own_bias_ref.shape[1]
    per_dev = positions // KB
    wide = rem_bias_ref.shape[-1]
    rows = per_group * positions
    chunks = (device + 1) // 2
    scaling = HD ** (-0.5)
    contract = (((1,), (1,)), ((), ()))

    def masked(scores, bias):
        width = scores.shape[-1]
        shaped = (scores * scaling).reshape(per_group, per_dev, KB, width)
        return (shaped + bias[None, :, None, :]).reshape(rows, width)

    @pl.loop(0, batch_size)
    def _(b):
        live = length_ref[b] - device * positions
        here = pl.ds(pl.multiple_of(b * positions, positions), positions)

        @pl.when(live <= 0)
        def _():
            out_ref[here, :] = jnp.zeros((positions, out_ref.shape[1]), out_ref.dtype)

        @pl.when(live > 0)
        def _():
            at_row = lax.broadcasted_iota(jnp.int32, (positions, positions), 0)
            at_col = lax.broadcasted_iota(jnp.int32, (positions, positions), 1)
            before, same = [
                jnp.broadcast_to(own_bias_ref[i, b][:, None, :], (per_dev, KB, positions)).reshape(
                    positions, positions
                )
                for i in range(2)
            ]
            own_bias = jnp.where(
                at_col < at_row, before, jnp.where(at_col == at_row, same, MASKED)
            )
            living = lax.broadcasted_iota(jnp.int32, (positions, HD), 0) < live
            for h in range(kv_local):
                cols = slice(h * HD, (h + 1) * HD)
                heads = [h * per_group + g for g in range(per_group)]
                queries = jnp.concatenate(
                    [q_ref[here, n * HD:(n + 1) * HD] for n in heads], axis=0
                )
                own = lax.dot_general(
                    queries, k_ref[here, cols], contract, preferred_element_type=jnp.float32
                )
                own = (own * scaling).reshape(per_group, positions, positions) + own_bias[None]
                own = own.reshape(rows, positions)
                top = jnp.max(own, axis=-1, keepdims=True)

                def score(c, top):
                    there = pl.ds(pl.multiple_of(c * wide, wide), wide)
                    far = lax.dot_general(
                        queries, rk_ref[there, cols], contract,
                        preferred_element_type=jnp.float32,
                    )
                    far = masked(far, rem_bias_ref[c, b])
                    scores_ref[c] = far
                    return jnp.maximum(top, jnp.max(far, axis=-1, keepdims=True))

                top = lax.fori_loop(0, chunks, score, top)
                raised = jnp.exp(own - top)
                total = jnp.sum(raised, axis=-1, keepdims=True)
                mixed = jnp.dot(
                    raised.astype(jnp.bfloat16), v_ref[here, cols],
                    preferred_element_type=jnp.float32,
                )

                def gather(c, carry):
                    total, mixed = carry
                    there = pl.ds(pl.multiple_of(c * wide, wide), wide)
                    raised = jnp.exp(scores_ref[c] - top)
                    total = total + jnp.sum(raised, axis=-1, keepdims=True)
                    mixed = mixed + jnp.dot(
                        raised.astype(jnp.bfloat16), rv_ref[there, cols],
                        preferred_element_type=jnp.float32,
                    )
                    return total, mixed

                total, mixed = lax.fori_loop(0, chunks, gather, (total, mixed))
                mixed = mixed / total
                for g, n in enumerate(heads):
                    part = mixed[g * positions:(g + 1) * positions]
                    out_ref[here, n * HD:(n + 1) * HD] = jnp.where(living, part, 0.0).astype(
                        out_ref.dtype
                    )


def attend(positions, kv_local, per_group, lengths, queries, k, v, rk, rv, own_bias, rem_bias):
    vmem = pl.BlockSpec(memory_space=pltpu.VMEM)
    return pl.pallas_call(
        functools.partial(attend_kernel, positions, kv_local, per_group),
        out_shape=jax.ShapeDtypeStruct(queries.shape, jnp.bfloat16),
        in_specs=[pl.BlockSpec(memory_space=pltpu.SMEM)] + [vmem] * 7,
        out_specs=vmem,
        scratch_shapes=[
            pltpu.VMEM(
                (rem_bias.shape[0], per_group * positions, rem_bias.shape[-1]), jnp.float32
            )
        ],
        compiler_params=pltpu.CompilerParams(vmem_limit_bytes=48 * 2**20),
    )(lengths, queries, k, v, rk, rv, own_bias, rem_bias)


def shards(inputs, query_weight, key_weight, value_weight, out_weight, chosen, lengths):
    batch_size, positions, model_width = inputs.shape
    kv_local = key_weight.shape[1] // HD
    heads_local = query_weight.shape[1] // HD
    per_group = heads_local // kv_local
    owned = batch_size * (positions // KB)
    device = lax.axis_index("kv")
    devices = lax.axis_size("kv")
    flat_rows = inputs.reshape(batch_size * positions, model_width)

    def project(weight):
        return jnp.dot(flat_rows, weight, preferred_element_type=jnp.float32).astype(jnp.bfloat16)

    queries = project(query_weight)
    key_rows = project(key_weight)
    value_rows = project(value_weight)
    requests, own_bias, rem_bias = tables(chosen, devices, device)
    asked = lax.all_to_all(requests, "kv", split_axis=0, concat_axis=0, tiled=True)

    def fetch(table):
        picked = table.reshape(owned, KB, kv_local * HD)[asked]
        got = lax.all_to_all(picked, "kv", split_axis=0, concat_axis=0, tiled=True)
        return got.reshape(devices * CAP * KB, kv_local * HD)

    attended = attend(
        positions, kv_local, per_group, lengths, queries, key_rows, value_rows,
        fetch(key_rows), fetch(value_rows), own_bias, rem_bias,
    )
    partial_value = jnp.dot(attended, out_weight, preferred_element_type=jnp.float32).astype(
        jnp.bfloat16
    )
    partial_value = partial_value.reshape(batch_size, positions, model_width)
    return lax.psum_scatter(partial_value, "tp", scatter_dimension=2, tiled=True)


def solution(mesh):
    placed = (
        P(None, "kv", None),
        P(None, "tp"),
        P(None, "tp"),
        P(None, "tp"),
        P("tp", None),
        P(None, "kv", None),
        P(),
    )
    return jax.shard_map(
        shards, mesh=mesh, in_specs=placed, out_specs=P(None, "kv", "tp"), check_vma=False
    )
```

```python
import functools

import jax
import jax.numpy as jnp
from jax import lax
from jax.experimental import pallas as pl
from jax.experimental.pallas import tpu as pltpu
from jax.sharding import PartitionSpec as P

HD = 128
KB = 64
CAP = 3
MASKED = -1e30


def tables(chosen, devices, device):
    batch_size, per_dev, _ = chosen.shape
    blocks = jnp.arange(devices * per_dev, dtype=jnp.int32)
    named = jnp.any(chosen[..., None] == blocks, axis=2)
    named = named.reshape(batch_size, per_dev, devices, per_dev)
    own = jnp.sum(
        jnp.where(jnp.arange(devices)[None, None, :, None] == device, named, False), axis=2
    )
    needed = jnp.any(named, axis=1) & (jnp.arange(devices)[None, :, None] != device)
    needed = jnp.transpose(needed, (1, 0, 2)).reshape(devices, batch_size * per_dev)
    local = jnp.arange(batch_size * per_dev, dtype=jnp.int32)
    slots = jnp.sum(
        jnp.where(local[None, :, None] > local[None, None, :], needed[:, None, :], False),
        axis=2,
        dtype=jnp.int32,
    )
    matches = needed[:, :, None] & (slots[:, :, None] == jnp.arange(CAP, dtype=jnp.int32))
    requests = jnp.sum(jnp.where(matches, local[None, :, None], 0), axis=1)
    matches = matches.reshape(devices, batch_size, per_dev, CAP)
    matches = jnp.transpose(matches, (1, 0, 2, 3))
    remote = jnp.any(named[..., None] & matches[:, None], axis=3)
    own_bias = jnp.where(own > 0, 0.0, MASKED).astype(jnp.float32)
    own_bias = jnp.repeat(own_bias, KB, axis=-1)
    home = device * per_dev + jnp.arange(per_dev, dtype=jnp.int32)
    copies = jnp.sum(chosen == home[None, :, None], axis=-1, dtype=jnp.int32)
    same = jnp.log(jnp.maximum(copies, 1).astype(jnp.float32))
    same = jnp.broadcast_to(same[..., None], own_bias.shape)
    rem_bias = jnp.where(remote, 0.0, MASKED).astype(jnp.float32)
    rem_bias = rem_bias.reshape(batch_size, per_dev, devices // 2, 2 * CAP)
    rem_bias = jnp.repeat(jnp.transpose(rem_bias, (2, 0, 1, 3)), KB, axis=-1)
    return requests, jnp.stack([own_bias, same]), rem_bias


def attend_kernel(
    positions, kv_local, per_group, length_ref, q_ref, k_ref, v_ref, rk_ref, rv_ref,
    own_bias_ref, rem_bias_ref, out_ref, scores_ref
):
    device = lax.axis_index("kv")
    batch_size = own_bias_ref.shape[1]
    per_dev = positions // KB
    wide = rem_bias_ref.shape[-1]
    rows = per_group * positions
    chunks = (device + 1) // 2
    scaling = HD ** (-0.5)
    contract = (((1,), (1,)), ((), ()))

    def masked(scores, bias):
        width = scores.shape[-1]
        shaped = (scores * scaling).reshape(per_group, per_dev, KB, width)
        return (shaped + bias[None, :, None, :]).reshape(rows, width)

    @pl.loop(0, batch_size)
    def _(b):
        live = length_ref[b] - device * positions
        here = pl.ds(pl.multiple_of(b * positions, positions), positions)

        @pl.when(live <= 0)
        def _():
            out_ref[here, :] = jnp.zeros((positions, out_ref.shape[1]), out_ref.dtype)

        @pl.when(live > 0)
        def _():
            at_row = lax.broadcasted_iota(jnp.int32, (positions, positions), 0)
            at_col = lax.broadcasted_iota(jnp.int32, (positions, positions), 1)
            before, same = [
                jnp.broadcast_to(own_bias_ref[i, b][:, None, :], (per_dev, KB, positions)).reshape(
                    positions, positions
                )
                for i in range(2)
            ]
            own_bias = jnp.where(
                at_col < at_row, before, jnp.where(at_col == at_row, same, MASKED)
            )
            living = lax.broadcasted_iota(jnp.int32, (positions, HD), 0) < live
            for h in range(kv_local):
                cols = slice(h * HD, (h + 1) * HD)
                heads = [h * per_group + g for g in range(per_group)]
                queries = jnp.concatenate(
                    [q_ref[here, n * HD:(n + 1) * HD] for n in heads], axis=0
                )
                own = lax.dot_general(
                    queries, k_ref[here, cols], contract, preferred_element_type=jnp.float32
                )
                own = (own * scaling).reshape(per_group, positions, positions) + own_bias[None]
                own = own.reshape(rows, positions)
                top = jnp.max(own, axis=-1, keepdims=True)

                def score(c, top):
                    there = pl.ds(pl.multiple_of(c * wide, wide), wide)
                    far = lax.dot_general(
                        queries, rk_ref[there, cols], contract,
                        preferred_element_type=jnp.float32,
                    )
                    far = masked(far, rem_bias_ref[c, b])
                    scores_ref[c] = far
                    return jnp.maximum(top, jnp.max(far, axis=-1, keepdims=True))

                top = lax.fori_loop(0, chunks, score, top)
                raised = jnp.exp(own - top)
                total = jnp.sum(raised, axis=-1, keepdims=True)
                mixed = jnp.dot(
                    raised.astype(jnp.bfloat16), v_ref[here, cols],
                    preferred_element_type=jnp.float32,
                )

                def gather(c, carry):
                    total, mixed = carry
                    there = pl.ds(pl.multiple_of(c * wide, wide), wide)
                    raised = jnp.exp(scores_ref[c] - top)
                    total = total + jnp.sum(raised, axis=-1, keepdims=True)
                    mixed = mixed + jnp.dot(
                        raised.astype(jnp.bfloat16), rv_ref[there, cols],
                        preferred_element_type=jnp.float32,
                    )
                    return total, mixed

                total, mixed = lax.fori_loop(0, chunks, gather, (total, mixed))
                mixed = mixed / total
                for g, n in enumerate(heads):
                    part = mixed[g * positions:(g + 1) * positions]
                    out_ref[here, n * HD:(n + 1) * HD] = jnp.where(living, part, 0.0).astype(
                        out_ref.dtype
                    )


def attend(positions, kv_local, per_group, lengths, queries, k, v, rk, rv, own_bias, rem_bias):
    vmem = pl.BlockSpec(memory_space=pltpu.VMEM)
    return pl.pallas_call(
        functools.partial(attend_kernel, positions, kv_local, per_group),
        out_shape=jax.ShapeDtypeStruct(queries.shape, jnp.bfloat16),
        in_specs=[pl.BlockSpec(memory_space=pltpu.SMEM)] + [vmem] * 7,
        out_specs=vmem,
        scratch_shapes=[
            pltpu.VMEM(
                (rem_bias.shape[0], per_group * positions, rem_bias.shape[-1]), jnp.float32
            )
        ],
        compiler_params=pltpu.CompilerParams(vmem_limit_bytes=48 * 2**20),
    )(lengths, queries, k, v, rk, rv, own_bias, rem_bias)


def mix_kernel(
    steps, tp, att_ref, weight_ref, out_ref,
    pair_out, pair_in, far_out, far_in, near,
    pair_sent, pair_got, far_sent, far_got,
):
    me = lax.axis_index("tp")
    core = lax.rem(me, 2)
    chip = me // 2
    chips = tp // 2
    partner = me + 1 - 2 * core
    width = out_ref.shape[1]
    step_rows = out_ref.shape[0] // steps
    mesh_id = pl.DeviceIdType.MESH

    def twin(off):
        return lax.rem(chip + off, chips) * 2 + core

    barrier = pltpu.get_barrier_semaphore()
    pl.semaphore_signal(barrier, inc=1, device_id={"tp": partner}, device_id_type=mesh_id)
    for off in range(1, chips):
        pl.semaphore_signal(barrier, inc=1, device_id={"tp": twin(off)}, device_id_type=mesh_id)
    pl.semaphore_wait(barrier, chips)

    def at(i):
        return pl.ds(pl.multiple_of(i * step_rows, step_rows), step_rows)

    def group_sum(i, off, side):
        column = (lax.rem(chip + off, chips) * 2 + side) * width
        return jnp.dot(
            att_ref[at(i), :],
            weight_ref[:, pl.ds(pl.multiple_of(column, width), width)],
            preferred_element_type=jnp.float32,
        ).astype(jnp.bfloat16)

    def pair_copy(i):
        return pltpu.make_async_remote_copy(
            src_ref=pair_out.at[i], dst_ref=pair_in.at[i],
            send_sem=pair_sent.at[i], recv_sem=pair_got.at[i],
            device_id={"tp": partner}, device_id_type=mesh_id,
        )

    def far_copy(i, off):
        return pltpu.make_async_remote_copy(
            src_ref=far_out.at[off - 1, i], dst_ref=far_in.at[off - 1, i],
            send_sem=far_sent.at[off - 1, i], recv_sem=far_got.at[off - 1, i],
            device_id={"tp": twin(off)}, device_id_type=mesh_id,
        )

    def step(i, carry):
        @pl.when(i < steps)
        def _():
            for off in range(chips):
                pair_out[i, off] = group_sum(i, off, 1 - core)
            pair_copy(i).start()

        @pl.when(i > 0)
        def _():
            j = i - 1
            sums = [group_sum(j, off, core).astype(jnp.float32) for off in range(chips)]
            pair_copy(j).wait_recv()
            for off in range(1, chips):
                both = sums[off] + pair_in[j, off].astype(jnp.float32)
                far_out[off - 1, j] = both.astype(jnp.bfloat16)
                far_copy(j, off).start()
            near[j] = sums[0] + pair_in[j, 0].astype(jnp.float32)

        return carry

    lax.fori_loop(0, steps + 1, step, 0)

    def finish(i, carry):
        pair_copy(i).wait_send()
        mixed = near[i]
        for off in range(1, chips):
            far_copy(i, off).wait()
            mixed = mixed + far_in[off - 1, i].astype(jnp.float32)
        out_ref[at(i), :] = mixed.astype(out_ref.dtype)
        return carry

    lax.fori_loop(0, steps, finish, 0)


def mix(attended, out_weight, tp):
    rows = attended.shape[0]
    width = out_weight.shape[1] // tp
    chips = tp // 2
    steps = rows // 128
    vmem = pl.BlockSpec(memory_space=pltpu.VMEM)
    pair = pltpu.VMEM((steps, chips, rows // steps, width), jnp.bfloat16)
    far = pltpu.VMEM((chips - 1, steps, rows // steps, width), jnp.bfloat16)
    return pl.pallas_call(
        functools.partial(mix_kernel, steps, tp),
        out_shape=jax.ShapeDtypeStruct((rows, width), jnp.bfloat16),
        in_specs=[vmem, vmem],
        out_specs=vmem,
        scratch_shapes=[
            pair, pair, far, far,
            pltpu.VMEM((steps, rows // steps, width), jnp.float32),
            pltpu.SemaphoreType.DMA((steps,)),
            pltpu.SemaphoreType.DMA((steps,)),
            pltpu.SemaphoreType.DMA((chips - 1, steps)),
            pltpu.SemaphoreType.DMA((chips - 1, steps)),
        ],
        compiler_params=pltpu.CompilerParams(
            collective_id=0, has_side_effects=True, vmem_limit_bytes=48 * 2**20
        ),
    )(attended, out_weight)


def shards(inputs, query_weight, key_weight, value_weight, out_weight, chosen, lengths):
    batch_size, positions, model_width = inputs.shape
    kv_local = key_weight.shape[1] // HD
    heads_local = query_weight.shape[1] // HD
    per_group = heads_local // kv_local
    owned = batch_size * (positions // KB)
    device = lax.axis_index("kv")
    devices = lax.axis_size("kv")
    flat_rows = inputs.reshape(batch_size * positions, model_width)

    def project(weight):
        return jnp.dot(flat_rows, weight, preferred_element_type=jnp.float32).astype(jnp.bfloat16)

    queries = project(query_weight)
    key_rows = project(key_weight)
    value_rows = project(value_weight)
    requests, own_bias, rem_bias = tables(chosen, devices, device)
    asked = lax.all_to_all(requests, "kv", split_axis=0, concat_axis=0, tiled=True)

    def fetch(table):
        picked = table.reshape(owned, KB, kv_local * HD)[asked]
        got = lax.all_to_all(picked, "kv", split_axis=0, concat_axis=0, tiled=True)
        return got.reshape(devices * CAP * KB, kv_local * HD)

    attended = attend(
        positions, kv_local, per_group, lengths, queries, key_rows, value_rows,
        fetch(key_rows), fetch(value_rows), own_bias, rem_bias,
    )
    mixed = mix(attended, out_weight, lax.axis_size("tp"))
    return mixed.reshape(batch_size, positions, -1)


def solution(mesh):
    placed = (
        P(None, "kv", None),
        P(None, "tp"),
        P(None, "tp"),
        P(None, "tp"),
        P("tp", None),
        P(None, "kv", None),
        P(),
    )
    return jax.shard_map(
        shards, mesh=mesh, in_specs=placed, out_specs=P(None, "kv", "tp"), check_vma=False
    )
```

```python
import functools

import jax
import jax.numpy as jnp
from jax import lax
from jax.experimental import pallas as pl
from jax.experimental.pallas import tpu as pltpu
from jax.sharding import PartitionSpec as P

HD = 128
KB = 64
CAP = 3
MASKED = -1e30


def tables(chosen, devices, device):
    batch_size, per_dev, _ = chosen.shape
    blocks = jnp.arange(devices * per_dev, dtype=jnp.int32)
    named = jnp.any(chosen[..., None] == blocks, axis=2)
    named = named.reshape(batch_size, per_dev, devices, per_dev)
    own = jnp.sum(
        jnp.where(jnp.arange(devices)[None, None, :, None] == device, named, False), axis=2
    )
    needed = jnp.any(named, axis=1) & (jnp.arange(devices)[None, :, None] != device)
    needed = jnp.transpose(needed, (1, 0, 2)).reshape(devices, batch_size * per_dev)
    local = jnp.arange(batch_size * per_dev, dtype=jnp.int32)
    slots = jnp.sum(
        jnp.where(local[None, :, None] > local[None, None, :], needed[:, None, :], False),
        axis=2,
        dtype=jnp.int32,
    )
    matches = needed[:, :, None] & (slots[:, :, None] == jnp.arange(CAP, dtype=jnp.int32))
    requests = jnp.sum(jnp.where(matches, local[None, :, None], 0), axis=1)
    matches = matches.reshape(devices, batch_size, per_dev, CAP)
    matches = jnp.transpose(matches, (1, 0, 2, 3))
    remote = jnp.any(named[..., None] & matches[:, None], axis=3)
    own_bias = jnp.where(own > 0, 0.0, MASKED).astype(jnp.float32)
    own_bias = jnp.repeat(own_bias, KB, axis=-1)
    home = device * per_dev + jnp.arange(per_dev, dtype=jnp.int32)
    copies = jnp.sum(chosen == home[None, :, None], axis=-1, dtype=jnp.int32)
    same = jnp.log(jnp.maximum(copies, 1).astype(jnp.float32))
    same = jnp.broadcast_to(same[..., None], own_bias.shape)
    rem_bias = jnp.where(remote, 0.0, MASKED).astype(jnp.float32)
    rem_bias = rem_bias.reshape(batch_size, per_dev, devices // 2, 2 * CAP)
    rem_bias = jnp.repeat(jnp.transpose(rem_bias, (2, 0, 1, 3)), KB, axis=-1)
    return requests, jnp.stack([own_bias, same]), rem_bias


def attend_kernel(
    positions, kv_local, per_group, length_ref, q_ref, k_ref, v_ref, rem_ref,
    own_bias_ref, rem_bias_ref, out_ref, scores_ref
):
    device = lax.axis_index("kv")
    batch_size = own_bias_ref.shape[1]
    per_dev = positions // KB
    wide = rem_bias_ref.shape[-1]
    rows = per_group * positions
    chunks = (device + 1) // 2
    scaling = HD ** (-0.5)
    contract = (((1,), (1,)), ((), ()))

    def masked(scores, bias):
        width = scores.shape[-1]
        shaped = (scores * scaling).reshape(per_group, per_dev, KB, width)
        return (shaped + bias[None, :, None, :]).reshape(rows, width)

    @pl.loop(0, batch_size)
    def _(b):
        live = length_ref[b] - device * positions
        here = pl.ds(pl.multiple_of(b * positions, positions), positions)

        @pl.when(live <= 0)
        def _():
            out_ref[here, :] = jnp.zeros((positions, out_ref.shape[1]), out_ref.dtype)

        @pl.when(live > 0)
        def _():
            at_row = lax.broadcasted_iota(jnp.int32, (positions, positions), 0)
            at_col = lax.broadcasted_iota(jnp.int32, (positions, positions), 1)
            before, same = [
                jnp.broadcast_to(own_bias_ref[i, b][:, None, :], (per_dev, KB, positions)).reshape(
                    positions, positions
                )
                for i in range(2)
            ]
            own_bias = jnp.where(
                at_col < at_row, before, jnp.where(at_col == at_row, same, MASKED)
            )
            living = lax.broadcasted_iota(jnp.int32, (positions, HD), 0) < live
            for h in range(kv_local):
                cols = slice(h * HD, (h + 1) * HD)
                far_cols = slice((kv_local + h) * HD, (kv_local + h + 1) * HD)
                heads = [h * per_group + g for g in range(per_group)]
                queries = jnp.concatenate(
                    [q_ref[here, n * HD:(n + 1) * HD] for n in heads], axis=0
                )
                own = lax.dot_general(
                    queries, k_ref[here, cols], contract, preferred_element_type=jnp.float32
                )
                own = (own * scaling).reshape(per_group, positions, positions) + own_bias[None]
                own = own.reshape(rows, positions)
                top = jnp.max(own, axis=-1, keepdims=True)

                def score(c, top):
                    there = pl.ds(pl.multiple_of(c * wide, wide), wide)
                    far = lax.dot_general(
                        queries, rem_ref[there, cols], contract,
                        preferred_element_type=jnp.float32,
                    )
                    far = masked(far, rem_bias_ref[c, b])
                    scores_ref[c] = far
                    return jnp.maximum(top, jnp.max(far, axis=-1, keepdims=True))

                top = lax.fori_loop(0, chunks, score, top)
                raised = jnp.exp(own - top)
                total = jnp.sum(raised, axis=-1, keepdims=True)
                mixed = jnp.dot(
                    raised.astype(jnp.bfloat16), v_ref[here, cols],
                    preferred_element_type=jnp.float32,
                )

                def gather(c, carry):
                    total, mixed = carry
                    there = pl.ds(pl.multiple_of(c * wide, wide), wide)
                    raised = jnp.exp(scores_ref[c] - top)
                    total = total + jnp.sum(raised, axis=-1, keepdims=True)
                    mixed = mixed + jnp.dot(
                        raised.astype(jnp.bfloat16), rem_ref[there, far_cols],
                        preferred_element_type=jnp.float32,
                    )
                    return total, mixed

                total, mixed = lax.fori_loop(0, chunks, gather, (total, mixed))
                mixed = mixed / total
                for g, n in enumerate(heads):
                    part = mixed[g * positions:(g + 1) * positions]
                    out_ref[here, n * HD:(n + 1) * HD] = jnp.where(living, part, 0.0).astype(
                        out_ref.dtype
                    )


def attend(positions, kv_local, per_group, lengths, queries, k, v, rem, own_bias, rem_bias):
    vmem = pl.BlockSpec(memory_space=pltpu.VMEM)
    return pl.pallas_call(
        functools.partial(attend_kernel, positions, kv_local, per_group),
        out_shape=jax.ShapeDtypeStruct(queries.shape, jnp.bfloat16),
        in_specs=[pl.BlockSpec(memory_space=pltpu.SMEM)] + [vmem] * 6,
        out_specs=vmem,
        scratch_shapes=[
            pltpu.VMEM(
                (rem_bias.shape[0], per_group * positions, rem_bias.shape[-1]), jnp.float32
            )
        ],
        compiler_params=pltpu.CompilerParams(vmem_limit_bytes=48 * 2**20),
    )(lengths, queries, k, v, rem, own_bias, rem_bias)


def mix_kernel(
    steps, tp, att_ref, weight_ref, out_ref,
    pair_out, pair_in, far_out, far_in, near,
    pair_sent, pair_got, far_sent, far_got,
):
    me = lax.axis_index("tp")
    core = lax.rem(me, 2)
    chip = me // 2
    chips = tp // 2
    partner = me + 1 - 2 * core
    width = out_ref.shape[1]
    step_rows = out_ref.shape[0] // steps
    mesh_id = pl.DeviceIdType.MESH

    def twin(off):
        return lax.rem(chip + off, chips) * 2 + core

    barrier = pltpu.get_barrier_semaphore()
    pl.semaphore_signal(barrier, inc=1, device_id={"tp": partner}, device_id_type=mesh_id)
    for off in range(1, chips):
        pl.semaphore_signal(barrier, inc=1, device_id={"tp": twin(off)}, device_id_type=mesh_id)
    pl.semaphore_wait(barrier, chips)

    def at(i):
        return pl.ds(pl.multiple_of(i * step_rows, step_rows), step_rows)

    def group_sum(i, off, side):
        column = (lax.rem(chip + off, chips) * 2 + side) * width
        return jnp.dot(
            att_ref[at(i), :],
            weight_ref[:, pl.ds(pl.multiple_of(column, width), width)],
            preferred_element_type=jnp.float32,
        ).astype(jnp.bfloat16)

    def pair_copy(i):
        return pltpu.make_async_remote_copy(
            src_ref=pair_out.at[i], dst_ref=pair_in.at[i],
            send_sem=pair_sent.at[i], recv_sem=pair_got.at[i],
            device_id={"tp": partner}, device_id_type=mesh_id,
        )

    def far_copy(i, off):
        return pltpu.make_async_remote_copy(
            src_ref=far_out.at[off - 1, i], dst_ref=far_in.at[off - 1, i],
            send_sem=far_sent.at[off - 1, i], recv_sem=far_got.at[off - 1, i],
            device_id={"tp": twin(off)}, device_id_type=mesh_id,
        )

    def step(i, carry):
        @pl.when(i < steps)
        def _():
            for off in range(chips):
                pair_out[i, off] = group_sum(i, off, 1 - core)
            pair_copy(i).start()

        @pl.when(i > 0)
        def _():
            j = i - 1
            sums = [group_sum(j, off, core).astype(jnp.float32) for off in range(chips)]
            pair_copy(j).wait_recv()
            for off in range(1, chips):
                both = sums[off] + pair_in[j, off].astype(jnp.float32)
                far_out[off - 1, j] = both.astype(jnp.bfloat16)
                far_copy(j, off).start()
            near[j] = sums[0] + pair_in[j, 0].astype(jnp.float32)

        return carry

    lax.fori_loop(0, steps + 1, step, 0)

    def finish(i, carry):
        pair_copy(i).wait_send()
        mixed = near[i]
        for off in range(1, chips):
            far_copy(i, off).wait()
            mixed = mixed + far_in[off - 1, i].astype(jnp.float32)
        out_ref[at(i), :] = mixed.astype(out_ref.dtype)
        return carry

    lax.fori_loop(0, steps, finish, 0)


def mix(attended, out_weight, tp):
    rows = attended.shape[0]
    width = out_weight.shape[1] // tp
    chips = tp // 2
    steps = rows // 128
    vmem = pl.BlockSpec(memory_space=pltpu.VMEM)
    pair = pltpu.VMEM((steps, chips, rows // steps, width), jnp.bfloat16)
    far = pltpu.VMEM((chips - 1, steps, rows // steps, width), jnp.bfloat16)
    return pl.pallas_call(
        functools.partial(mix_kernel, steps, tp),
        out_shape=jax.ShapeDtypeStruct((rows, width), jnp.bfloat16),
        in_specs=[vmem, vmem],
        out_specs=vmem,
        scratch_shapes=[
            pair, pair, far, far,
            pltpu.VMEM((steps, rows // steps, width), jnp.float32),
            pltpu.SemaphoreType.DMA((steps,)),
            pltpu.SemaphoreType.DMA((steps,)),
            pltpu.SemaphoreType.DMA((chips - 1, steps)),
            pltpu.SemaphoreType.DMA((chips - 1, steps)),
        ],
        compiler_params=pltpu.CompilerParams(
            collective_id=0, has_side_effects=True, vmem_limit_bytes=48 * 2**20
        ),
    )(attended, out_weight)


def shards(inputs, query_weight, key_weight, value_weight, out_weight, chosen, lengths):
    batch_size, positions, model_width = inputs.shape
    kv_local = key_weight.shape[1] // HD
    heads_local = query_weight.shape[1] // HD
    per_group = heads_local // kv_local
    owned = batch_size * (positions // KB)
    device = lax.axis_index("kv")
    devices = lax.axis_size("kv")
    flat_rows = inputs.reshape(batch_size * positions, model_width)

    def project(weight):
        return jnp.dot(flat_rows, weight, preferred_element_type=jnp.float32).astype(jnp.bfloat16)

    queries = project(query_weight)
    key_rows = project(key_weight)
    value_rows = project(value_weight)
    requests, own_bias, rem_bias = tables(chosen, devices, device)
    asked = lax.all_to_all(requests, "kv", split_axis=0, concat_axis=0, tiled=True)

    picked = jnp.concatenate(
        [
            table.reshape(owned, KB, kv_local * HD)[asked]
            for table in (key_rows, value_rows)
        ],
        axis=-1,
    )
    got = lax.all_to_all(picked, "kv", split_axis=0, concat_axis=0, tiled=True)
    got = got.reshape(devices * CAP * KB, 2 * kv_local * HD)
    attended = attend(
        positions, kv_local, per_group, lengths, queries, key_rows, value_rows,
        got, own_bias, rem_bias,
    )
    mixed = mix(attended, out_weight, lax.axis_size("tp"))
    return mixed.reshape(batch_size, positions, -1)


def solution(mesh):
    placed = (
        P(None, "kv", None),
        P(None, "tp"),
        P(None, "tp"),
        P(None, "tp"),
        P("tp", None),
        P(None, "kv", None),
        P(),
    )
    return jax.shard_map(
        shards, mesh=mesh, in_specs=placed, out_specs=P(None, "kv", "tp"), check_vma=False
    )
```
